32 devices in a mesh: sp: 8 (over z, y), dp: 4 (over x, core).
Axes of the slice: x: 2, y: 2, z: 4, core: 2. Of those that a mesh axis runs over, the one named last changes fastest.
Arguments:
- skip_connection_stream: bfloat16 [4, 1024, 2048], P('dp', 'sp'), may hold values from -6 to 6
- emitted_valve_unscaled: bfloat16 [4, 1024, 1024], P('dp', 'sp'), may hold values from -6 to 6
- channel_source_mapped: bfloat16 [4, 1024, 1024], P('dp', 'sp'), may hold values from -6 to 6
- hidden_source_mapped: bfloat16 [4, 1024, 256], P('dp', 'sp'), may hold values from -6 to 6
- probe_mapped_values: bfloat16 [4, 1024, 256], P('dp', 'sp'), may hold values from -6 to 6
- increment_premapped: float32 [4, 1024, 16], P('dp', None, 'sp'), may hold values from -6 to 6
- extra_log_fading: float32 [4, 1024, 16], P('dp', None, 'sp'), may hold values from -2 to 0
- channel_fading_speed: float32 [16], replicated, may hold values from 0 to 1, as said below
- channel_source_kernel: float32 [4, 1024], replicated, may hold values from -3 to 3
- hidden_source_kernel: float32 [4, 256], replicated, may hold values from -3 to 3
- probe_kernel_coefficients: float32 [4, 256], replicated, may hold values from -3 to 3
- cluster_scaling_factor: float32 [1024], replicated, may hold values from 0.1 to 1.9
- emitted_mapping_matrix: bfloat16 [1024, 2048], replicated, may hold values from -0.1875 to 0.1875
- standardize_scaling: float32 [2048], replicated, may hold values from 0.1 to 1.9
- standardize_offset: float32 [2048], replicated, may hold values from -2 to 2
- chosen_specialist_ids: int32 [4, 1024, 2], P('dp', 'sp'), may hold values from 0 to 7, all different within a row; in each aligned block of 128 rows (0 to 127, 128 to 255, ..., all dimensions but the last counted through in order) at most 48 rows name the same one
- specialist_mixing_shares: float32 [4, 1024, 2], P('dp', 'sp'), may hold values from 0.2 to 1
- specialist_gating_matrices: bfloat16 [8, 2048, 5120], P('sp', None, 'dp'), may hold values from -0.125 to 0.125
- raising_matrices: bfloat16 [8, 2048, 5120], P('sp', None, 'dp'), may hold values from -0.125 to 0.125
- lowering_matrices: bfloat16 [8, 5120, 2048], P('sp', 'dp'), may hold values from -0.078125 to 0.078125
Outputs:
- layer_out: bfloat16 [4, 1024, 2048], P('dp', 'sp')
The draws below stay inside these ranges and needn't reach their ends.
Inputs may be any that keep to these rules, and one draw needn't show every extreme that they name: `chosen_specialist_ids`: each row names two different experts. The rows of one device name no expert more than 48 times, a bound that some block reaches. `channel_fading_speed`: Positive.
All inputs are finite; a program needn't handle non-finite values.
Results may differ from the reference program's by a relative error of at most 0.015.
Values may be sent and summed in bfloat16 or wider, within the bound.
A program may use at most 128 MiB of HBM per device.

```python
import math
import jax
import jax.numpy as jnp
import numpy as np
from jax import lax

D = 2048
HEADS = 16
HEAD_DIM = 64
GROUPS = 4
STATE = 64
FF = 5120
KERNEL = 4
BLK = 128
TOK = 128
INNER = 1024
EXPERTS = 8
CAP = 48
FF_PART = 1280
LEN = 1024
BATCH = 4
N_SP = 8
N_DP = 4


def draw_increment_premapped(key, part):
    noise_key, shift_key = jax.random.split(key)
    block_count = LEN // TOK
    shifted = jax.random.uniform(shift_key, (BATCH, block_count, 1, HEADS), jnp.float32, -1.2, 1.2)
    noise = jax.random.normal(noise_key, (BATCH, block_count, TOK, HEADS), jnp.float32)
    return jnp.clip(noise + shifted, -6.0, 6.0).reshape(BATCH, LEN, HEADS)


def draw_extra_log_fading(key, part):
    spot_key, loss_key = jax.random.split(key)
    spots = jax.random.randint(spot_key, (BATCH, 1, HEADS, 2), 0, LEN)
    losses = jax.random.uniform(loss_key, (BATCH, 1, HEADS, 2), jnp.float32, 0.2, 0.5)
    matched = jnp.arange(LEN)[None, :, None, None] == spots
    return jnp.sum(jnp.where(matched, jnp.log(1.0 - losses), 0.0), axis=3)


def draw_channel_fading_speed(key, part):
    pick_key, fast_key, slow_key = jax.random.split(key, 3)
    fast_share = 0.5
    quick = jax.random.bernoulli(pick_key, fast_share, (HEADS,))
    fast_rate = jnp.exp(jax.random.uniform(fast_key, (HEADS,), jnp.float32, math.log(0.03), math.log(0.1))) / 0.8
    slow_rate = jnp.exp(jax.random.uniform(slow_key, (HEADS,), jnp.float32, math.log(0.2), math.log(0.8))) / (0.8 * LEN)
    return jnp.where(quick, fast_rate, slow_rate)


def block_scale(rng, extent, cuts, least, high):
    def one(dim, blocks):
        heights = jax.random.uniform(jax.random.fold_in(jax.random.fold_in(rng, 6), dim), (blocks,), jnp.float32, least / len(cuts), high / len(cuts))
        return jnp.repeat(jnp.exp(heights), extent[dim] // blocks).reshape((-1,) + (1,) * (len(extent) - dim - 1))

    gain = one(*cuts[0])
    for cut in cuts[1:]:
        gain = gain * one(*cut)
    return gain


def deal_out(stream_key, own, number, rows, number_of, top, reach, skew):
    sequence = jax.random.permutation(stream_key, number_of)
    crowded, common = portions_of(number_of, rows * top, reach, skew, True), portions_of(number_of, rows * top, reach, skew, False)
    places = jnp.arange(number_of)

    def named(lengths, rotation):
        used = int((lengths > 0).sum())
        fixed = max(1, used // 4)
        passed = fixed + (places - fixed + rotation * (used - fixed)) % max(1, number_of - fixed)
        return jnp.zeros((number_of,), jnp.int32).at[sequence[jnp.where(places < fixed, places, passed)]].set(jnp.asarray(lengths, jnp.int32))

    lengths = jnp.where(number % 4 == 0, named(crowded, number // 4), named(common, number - number // 4 - 1))
    mixed = jax.random.permutation(jax.random.fold_in(own, 3), number_of)
    donor, taker = mixed[0:number_of // 2 * 2:2], mixed[1:number_of // 2 * 2:2]
    room = jnp.minimum(lengths[donor] - 1, reach - lengths[taker]) // 2
    room = jnp.where((donor == sequence[0]) | (taker == sequence[0]) | (lengths[taker] == 0), 0, jnp.maximum(room, 0))
    passed = jax.random.randint(jax.random.fold_in(own, 4), (number_of // 2,), 0, 1 << 20) % (room + 1)
    lengths = lengths.at[donor].add(-passed).at[taker].add(passed)
    members = jnp.searchsorted(jnp.cumsum(lengths), jnp.arange(rows * top), side="right").astype(jnp.int32)
    grid = members.reshape(top, rows).T
    grid = grid[jax.random.permutation(jax.random.fold_in(own, 1), rows)]
    rotation = jax.random.randint(jax.random.fold_in(own, 2), (rows, 1), 0, top)
    return jnp.take_along_axis(grid, (jnp.arange(top)[None, :] + rotation) % top, axis=1)


def portions_of(amount, total, limit, lean, full):
    loads = [(1 << 20) // math.isqrt(grade ** lean) + 1 for grade in range(1, amount + 1)]
    largest = limit if full else min(limit, max(-(-total // amount), total * loads[0] // sum(loads)))
    least = 1 if total - largest >= amount - 1 else 0
    given, rest = [largest] + [least] * (amount - 1), total - largest - least * (amount - 1)
    while rest > 0:
        free = [i for i in range(1, amount) if given[i] < largest] or [i for i in range(1, amount) if given[i] < limit]
        whole, left = sum([loads[i] for i in free]), rest
        for i in free:
            more = min(limit - given[i], max(1, left * loads[i] // whole), rest)
            given[i] = given[i] + more
            rest = rest - more
    return np.array(given)


def bell_draw(rng, dims, scale, limit, cuts=(), held_as=jnp.bfloat16):
    array = scale * jax.random.normal(rng, dims, jnp.float32)
    if cuts:
        array = array * block_scale(rng, dims, cuts, -0.22, 0.18)
    return jnp.clip(array, -limit, limit).astype(held_as)


def setup_inputs(seed: int = 0) -> dict:
    key_list = jax.random.split(jax.random.key(seed), 21)
    skip_connection_stream = bell_draw(key_list[0], (BATCH, LEN, D), 1.0, 6.0, ((0, 4), (1, 8)))
    emitted_valve_unscaled = bell_draw(key_list[1], (BATCH, LEN, INNER), 1.0, 6.0, ((0, 4), (1, 8)))
    channel_source_mapped = bell_draw(key_list[2], (BATCH, LEN, INNER), 1.0, 6.0, ((0, 4), (1, 8)))
    hidden_source_mapped = bell_draw(key_list[3], (BATCH, LEN, GROUPS * STATE), 1.0, 6.0, ((0, 4), (1, 8)))
    probe_mapped_values = bell_draw(key_list[4], (BATCH, LEN, GROUPS * STATE), 1.0, 6.0, ((0, 4), (1, 8)))
    increment_premapped = draw_increment_premapped(jax.random.fold_in(key_list[20], 71), 0)
    extra_log_fading = draw_extra_log_fading(jax.random.fold_in(key_list[20], 71), 0)
    channel_fading_speed = draw_channel_fading_speed(jax.random.fold_in(key_list[20], 71), 0)
    channel_source_kernel = bell_draw(key_list[8], (KERNEL, INNER), KERNEL ** -0.5, 3.0, (), jnp.float32)
    hidden_source_kernel = bell_draw(key_list[9], (KERNEL, GROUPS * STATE), KERNEL ** -0.5, 3.0, (), jnp.float32)
    probe_kernel_coefficients = bell_draw(key_list[10], (KERNEL, GROUPS * STATE), KERNEL ** -0.5, 3.0, (), jnp.float32)
    cluster_scaling_factor = jnp.clip(1.0 + 0.18 * jax.random.normal(key_list[11], (INNER,), jnp.float32), 0.1, 1.9)
    emitted_mapping_matrix = bell_draw(key_list[12], (INNER, D), INNER ** -0.5, 0.1875)
    standardize_scaling = jnp.clip(1.0 + 0.18 * jax.random.normal(key_list[13], (D,), jnp.float32), 0.1, 1.9)
    standardize_offset = bell_draw(key_list[14], (D,), 0.3, 2.0, (), jnp.float32)
    chosen_specialist_ids_keys = jax.random.split(jax.random.fold_in(key_list[15], 1), BATCH * LEN // TOK)
    chosen_specialist_ids_turns = jax.random.permutation(jax.random.fold_in(key_list[15], 3), BATCH * LEN // TOK)
    chosen_specialist_ids = jax.vmap(lambda own, number: deal_out(jax.random.fold_in(key_list[15], 2), own, number, TOK, EXPERTS, 2, CAP, 2))(chosen_specialist_ids_keys, chosen_specialist_ids_turns).reshape((BATCH, LEN, 2))
    specialist_mixing_shares = jnp.clip(0.2 + 0.8 * jax.random.uniform(key_list[16], (BATCH, LEN, 2), jnp.float32) ** block_scale(key_list[16], (BATCH, LEN, 2), ((0, 4), (1, 8)), -0.2, 0.2), 0.2, 1.0)
    specialist_gating_matrices = bell_draw(key_list[17], (EXPERTS, D, FF), D ** -0.5, 0.125, ((0, 8), (2, 4)))
    raising_matrices = bell_draw(key_list[18], (EXPERTS, D, FF), D ** -0.5, 0.125, ((0, 8), (2, 4)))
    lowering_matrices = bell_draw(key_list[19], (EXPERTS, FF, D), FF ** -0.5, 0.078125, ((0, 8), (1, 4)))
    return dict(skip_connection_stream=skip_connection_stream, emitted_valve_unscaled=emitted_valve_unscaled, channel_source_mapped=channel_source_mapped, hidden_source_mapped=hidden_source_mapped, probe_mapped_values=probe_mapped_values, increment_premapped=increment_premapped, extra_log_fading=extra_log_fading, channel_fading_speed=channel_fading_speed, channel_source_kernel=channel_source_kernel, hidden_source_kernel=hidden_source_kernel, probe_kernel_coefficients=probe_kernel_coefficients, cluster_scaling_factor=cluster_scaling_factor, emitted_mapping_matrix=emitted_mapping_matrix, standardize_scaling=standardize_scaling, standardize_offset=standardize_offset, chosen_specialist_ids=chosen_specialist_ids, specialist_mixing_shares=specialist_mixing_shares, specialist_gating_matrices=specialist_gating_matrices, raising_matrices=raising_matrices, lowering_matrices=lowering_matrices)


rms_eps = 1e-06
norm_eps = 1e-05

def causal_conv(series, tap_weights, rim_rows):
    padded = jnp.concatenate([rim_rows, series], axis=0).astype(jnp.float32)
    length = series.shape[0]
    running = jnp.zeros(series.shape, jnp.float32)
    for tap_index in range(tap_weights.shape[0]):
        running = running + tap_weights[tap_index].astype(jnp.float32) * lax.slice_in_dim(padded, tap_index, tap_index + length, axis=0)
    return jax.nn.silu(running).astype(jnp.bfloat16)

def ssd_blocks(x_conv, b_conv, c_conv, increment_delta, fading_exponent, init_state, block_len):
    length, head_count, head_width = x_conv.shape
    state_width = b_conv.shape[2]
    block_count = length // block_len
    x_block = x_conv.reshape(block_count, block_len, head_count, head_width).astype(jnp.float32)
    b_block = b_conv.reshape(block_count, block_len, head_count, state_width).astype(jnp.float32)
    c_block = c_conv.reshape(block_count, block_len, head_count, state_width).astype(jnp.float32)
    cumulative = jnp.cumsum(jnp.transpose(fading_exponent.reshape(block_count, block_len, head_count), (0, 2, 1)), axis=2)
    step_heads = jnp.transpose(increment_delta.reshape(block_count, block_len, head_count), (0, 2, 1))
    causal = jnp.arange(block_len)[:, None] >= jnp.arange(block_len)[None, :]
    within = jnp.exp(jnp.where(causal, cumulative[:, :, :, None] - cumulative[:, :, None, :], -jnp.inf))
    scores = jnp.einsum('cthn,cshn->chts', c_block, b_block)
    mixing = (scores * within * step_heads[:, :, None, :]).astype(jnp.bfloat16)
    diag_out = jnp.einsum('chts,cshp->cthp', mixing.astype(jnp.float32), x_block)
    tail_decay = jnp.exp(cumulative[:, :, -1:] - cumulative) * step_heads
    scaled = (x_block * jnp.transpose(tail_decay, (0, 2, 1))[:, :, :, None]).astype(jnp.bfloat16)
    block_state = jnp.einsum('cshp,cshn->chpn', scaled.astype(jnp.float32), b_block)
    totals = cumulative[:, :, -1]
    through = jnp.cumsum(totals, axis=0)
    before = through - totals
    earlier = jnp.arange(block_count)[:, None] > jnp.arange(block_count)[None, :]
    carry_weight = jnp.exp(jnp.where(earlier[:, :, None], before[:, None, :] - through[None, :, :], -jnp.inf))
    entering = jnp.einsum('cjh,jhpn->chpn', carry_weight, block_state, precision=lax.Precision.HIGHEST) + jnp.exp(before)[:, :, None, None] * init_state[None]
    reach_decay = jnp.transpose(jnp.exp(cumulative), (0, 2, 1))
    carried_out = jnp.einsum('cthn,chpn->cthp', c_block, entering, precision=lax.Precision.HIGHEST) * reach_decay[:, :, :, None]
    outcome = (diag_out + carried_out).reshape(length, head_count, head_width)
    final_state = jnp.einsum('jh,jhpn->hpn', jnp.exp(through[-1][None, :] - through), block_state, precision=lax.Precision.HIGHEST) + jnp.exp(through[-1])[:, None, None] * init_state
    return (outcome, final_state, through[-1])

def reference(skip_connection_stream, emitted_valve_unscaled, channel_source_mapped, hidden_source_mapped, probe_mapped_values, increment_premapped, extra_log_fading, channel_fading_speed, channel_source_kernel, hidden_source_kernel, probe_kernel_coefficients, cluster_scaling_factor, emitted_mapping_matrix, standardize_scaling, standardize_offset, chosen_specialist_ids, specialist_mixing_shares, specialist_gating_matrices, raising_matrices, lowering_matrices):
    per_group = HEADS // GROUPS
    tap_weights = jnp.concatenate([channel_source_kernel, hidden_source_kernel, probe_kernel_coefficients], axis=1)

    def lone_token_list(token_segments):
        channel_source_list, hidden_source_list, probe_value_list, increment_list, extra_fading_list = token_segments
        joined_rows = jnp.concatenate([channel_source_list, hidden_source_list, probe_value_list], axis=1)
        rim_rows = jnp.zeros((KERNEL - 1, joined_rows.shape[1]), jnp.bfloat16)
        convolved = causal_conv(joined_rows, tap_weights, rim_rows)
        x_conv = convolved[:, :INNER].reshape(LEN, HEADS, HEAD_DIM)
        b_conv = jnp.repeat(convolved[:, INNER:INNER + GROUPS * STATE].reshape(LEN, GROUPS, STATE), per_group, axis=1)
        c_conv = jnp.repeat(convolved[:, INNER + GROUPS * STATE:].reshape(LEN, GROUPS, STATE), per_group, axis=1)
        increment_delta = jax.nn.softplus(increment_list)
        fading_exponent = extra_fading_list - channel_fading_speed[None, :] * increment_delta
        init_state = jnp.zeros((HEADS, HEAD_DIM, STATE), jnp.float32)
        outcome, final_state, total_decay = ssd_blocks(x_conv, b_conv, c_conv, increment_delta, fading_exponent, init_state, BLK)
        return outcome.reshape(LEN, INNER).astype(jnp.bfloat16)
    blending_outcome = lax.map(lone_token_list, (channel_source_mapped, hidden_source_mapped, probe_mapped_values, increment_premapped, extra_log_fading))
    all_rows = BATCH * LEN
    gated = blending_outcome.reshape(all_rows, INNER).astype(jnp.float32) * jax.nn.silu(emitted_valve_unscaled.reshape(all_rows, INNER).astype(jnp.float32))
    grouped = gated.reshape(all_rows, GROUPS, INNER // GROUPS)
    grouped = grouped * lax.rsqrt(lax.optimization_barrier(jnp.mean(grouped * grouped, axis=-1, keepdims=True)) + rms_eps)
    group_normed = (grouped.reshape(all_rows, INNER) * cluster_scaling_factor[None, :]).astype(jnp.bfloat16)
    pre_norm = skip_connection_stream.reshape(all_rows, D).astype(jnp.float32) + jnp.dot(group_normed, emitted_mapping_matrix, preferred_element_type=jnp.float32)
    centre = lax.optimization_barrier(jnp.mean(pre_norm, axis=-1, keepdims=True))
    variance = lax.optimization_barrier(jnp.mean(jnp.square(pre_norm - centre), axis=-1, keepdims=True))
    normed = ((pre_norm - centre) * lax.rsqrt(variance + norm_eps) * standardize_scaling[None, :] + standardize_offset[None, :]).astype(jnp.bfloat16)
    flat_ids = chosen_specialist_ids.reshape(-1).astype(jnp.int32)
    flat_weights = specialist_mixing_shares.reshape(-1).astype(jnp.float32)
    owner = (jnp.arange(all_rows * 2, dtype=jnp.int32) // 2).astype(jnp.int32)
    buffer_rows = N_SP * N_DP * CAP
    padded_rows = jnp.concatenate([normed, jnp.zeros((1, D), jnp.bfloat16)], axis=0)

    def one_expert(running, expert):
        matched = flat_ids == expert
        ranked = jnp.cumsum(matched.astype(jnp.int32)) - 1
        placed = jnp.where(matched, ranked, buffer_rows).astype(jnp.int32)
        source = jnp.full((buffer_rows + 1,), all_rows, jnp.int32).at[placed].set(owner)[:buffer_rows]
        weight_at = jnp.zeros((buffer_rows + 1,), jnp.float32).at[placed].set(flat_weights)[:buffer_rows]
        rows_in = padded_rows[source]
        gate_val = jnp.dot(rows_in, specialist_gating_matrices[expert], preferred_element_type=jnp.float32)
        up_val = jnp.dot(rows_in, raising_matrices[expert], preferred_element_type=jnp.float32)
        hidden = (jax.nn.silu(gate_val) * up_val).astype(jnp.bfloat16)
        expert_sum = jnp.zeros((buffer_rows, D), jnp.float32)
        for part_index in range(N_DP):
            lower = part_index * FF_PART
            partial_value = jnp.dot(hidden[:, lower:lower + FF_PART], lowering_matrices[expert, lower:lower + FF_PART], preferred_element_type=jnp.float32).astype(jnp.bfloat16)
            expert_sum = expert_sum + lax.optimization_barrier(partial_value).astype(jnp.float32)
        expert_out = expert_sum.astype(jnp.bfloat16)
        running = running.at[source].add(weight_at[:, None] * expert_out.astype(jnp.float32))
        return (running, None)
    routed_sum, unused = lax.scan(one_expert, jnp.zeros((all_rows + 1, D), jnp.float32), jnp.arange(EXPERTS, dtype=jnp.int32))
    layer_out = (normed.astype(jnp.float32) + routed_sum[:all_rows]).astype(jnp.bfloat16)
    return layer_out.reshape(BATCH, LEN, D)
```

```python
import functools

import jax
import jax.numpy as jnp
from jax import lax
from jax.experimental import pallas as pl
from jax.experimental.pallas import tpu as pltpu
from jax.sharding import PartitionSpec as P

HEADS = 16
HEAD_DIM = 64
GROUPS = 4
STATE = 64
KERNEL = 4
BLK = 128


rms_eps = 1e-06
norm_eps = 1e-05


def causal_conv(series, tap_weights, rim_rows):
    padded = jnp.concatenate([rim_rows, series], axis=0).astype(jnp.float32)
    length = series.shape[0]
    running = jnp.zeros(series.shape, jnp.float32)
    for tap_index in range(tap_weights.shape[0]):
        running = running + tap_weights[tap_index] * lax.slice_in_dim(
            padded, tap_index, tap_index + length, axis=0
        )
    return jax.nn.silu(running).astype(jnp.bfloat16)


def ssd_blocks(x_conv, b_conv, c_conv, increment_delta, fading_exponent, init_state, block_len):
    length, head_count, head_width = x_conv.shape
    state_width = b_conv.shape[2]
    block_count = length // block_len
    x_block = x_conv.reshape(block_count, block_len, head_count, head_width)
    b_block = b_conv.reshape(block_count, block_len, head_count, state_width)
    c_block = c_conv.reshape(block_count, block_len, head_count, state_width)
    cumulative = jnp.cumsum(
        jnp.transpose(fading_exponent.reshape(block_count, block_len, head_count), (0, 2, 1)),
        axis=2,
    )
    step_heads = jnp.transpose(
        increment_delta.reshape(block_count, block_len, head_count), (0, 2, 1)
    )
    causal = jnp.arange(block_len)[:, None] >= jnp.arange(block_len)[None, :]
    within = jnp.exp(
        jnp.where(causal, cumulative[:, :, :, None] - cumulative[:, :, None, :], -jnp.inf)
    )
    scores = jnp.einsum("cthn,cshn->chts", c_block, b_block, preferred_element_type=jnp.float32)
    mixing = (scores * within * step_heads[:, :, None, :]).astype(jnp.bfloat16)
    diag_out = jnp.einsum("chts,cshp->cthp", mixing, x_block, preferred_element_type=jnp.float32)
    tail_decay = jnp.exp(cumulative[:, :, -1:] - cumulative) * step_heads
    scaled = (
        x_block.astype(jnp.float32) * jnp.transpose(tail_decay, (0, 2, 1))[:, :, :, None]
    ).astype(jnp.bfloat16)
    block_state = jnp.einsum("cshp,cshn->chpn", scaled, b_block, preferred_element_type=jnp.float32)
    totals = cumulative[:, :, -1]
    through = jnp.cumsum(totals, axis=0)
    before = through - totals
    earlier = jnp.arange(block_count)[:, None] > jnp.arange(block_count)[None, :]
    carry_weight = jnp.exp(
        jnp.where(earlier[:, :, None], before[:, None, :] - through[None, :, :], -jnp.inf)
    )
    entering = (
        jnp.einsum("cjh,jhpn->chpn", carry_weight, block_state, precision=lax.Precision.HIGHEST)
        + jnp.exp(before)[:, :, None, None] * init_state[None]
    )
    reach_decay = jnp.transpose(jnp.exp(cumulative), (0, 2, 1))
    carried_out = (
        jnp.einsum(
            "cthn,chpn->cthp",
            c_block.astype(jnp.float32),
            entering,
            precision=lax.Precision.HIGHEST,
        )
        * reach_decay[:, :, :, None]
    )
    outcome = (diag_out + carried_out).reshape(length, head_count, head_width)
    final_state = (
        jnp.einsum(
            "jh,jhpn->hpn",
            jnp.exp(through[-1][None, :] - through),
            block_state,
            precision=lax.Precision.HIGHEST,
        )
        + jnp.exp(through[-1])[:, None, None] * init_state
    )
    return (outcome, final_state, through[-1])

MESH = pl.DeviceIdType.MESH


def flip(value, mask):
    result, bit = value, 1
    while bit <= mask:
        if mask & bit:
            result = result + bit * (1 - 2 * ((value // bit) % 2))
        bit *= 2
    return result


def expert_kernel(
    S, R, cap, group, out_ref, wg_hbm, wu_hbm, wd_hbm, ret_ref,
    arr, hid, ra, rx, sx, fin, wg, wu, wd,
    wsem, own_sem, d_s, d_r, g_s, g_r, a_s, a_r, x_s, x_r, b_s, b_r,
):
    s = lax.axis_index("sp")
    d = lax.axis_index("dp")
    nx = R // 2
    steps = S // group
    order = [0] + list(range(steps - 1, 0, -1))
    members = [[p * group + i for i in range(group)] for p in order]
    width = wd.shape[1]
    ff = wg.shape[1]
    f32 = jnp.float32

    def rows(j, dc, dx, count=1):
        return pl.ds((j * R + dc * nx + dx) * cap, count * cap)

    def remote(src, dst, send, recv, where):
        return pltpu.make_async_remote_copy(
            src_ref=src, dst_ref=dst, send_sem=send, recv_sem=recv,
            device_id=where, device_id_type=MESH,
        )

    def disp(j):
        return remote(out_ref.at[pl.ds(j * cap, cap)], arr.at[rows(j, 0, 0)],
                      d_s.at[j], d_r.at[j], {"sp": flip(s, j)})

    def agx(j, dx):
        return remote(arr.at[rows(j, 0, 0)], arr.at[rows(j, 0, dx)],
                      g_s.at[j, dx], g_r.at[j, dx], {"dp": flip(d, 2 * dx)})

    def agc(j, dx):
        return remote(arr.at[rows(j, 0, dx)], arr.at[rows(j, 1, dx)],
                      g_s.at[j, nx + dx], g_r.at[j, nx + dx], {"dp": flip(d, 1)})

    def rsc(j):
        return remote(arr.at[rows(j, 1, 0, nx)], ra.at[pl.ds(j * nx * cap, nx * cap)],
                      a_s.at[j], a_r.at[j], {"dp": flip(d, 1)})

    def rsx(j, dx):
        at = pl.ds((j * (nx - 1) + dx - 1) * cap, cap)
        return remote(sx.at[at], rx.at[at], x_s.at[j, dx], x_r.at[j, dx], {"dp": flip(d, 2 * dx)})

    def back(j):
        return remote(fin.at[pl.ds(j * cap, cap)], ret_ref.at[pl.ds(j * cap, cap)],
                      b_s.at[j], b_r.at[j], {"sp": flip(s, j)})

    own = pltpu.make_async_copy(out_ref.at[pl.ds(0, cap)], arr.at[rows(0, 0, 0)], own_sem)
    loads = [
        pltpu.make_async_copy(src, dst, wsem.at[i])
        for i, (src, dst) in enumerate(((wg_hbm, wg), (wu_hbm, wu), (wd_hbm, wd)))
    ]
    own.start()
    for load in loads:
        load.start()

    barrier = pltpu.get_barrier_semaphore()
    peers = [{"sp": flip(s, j)} for j in range(1, S)]
    peers += [{"dp": flip(d, 1)}] + [{"dp": flip(d, 2 * dx)} for dx in range(1, nx)]
    for peer in peers:
        pl.semaphore_signal(barrier, inc=1, device_id=peer, device_id_type=MESH)
    pl.semaphore_wait(barrier, len(peers))

    for js in members:
        for j in js:
            if j:
                disp(j).start()

    def arrive(p):
        for j in members[p]:
            if j:
                disp(j).wait_recv()
            else:
                own.wait()
            for dx in range(1, nx):
                agx(j, dx).start()
            agc(j, 0).start()

    def relay(p):
        for j in members[p]:
            for dx in range(1, nx):
                agx(j, dx).wait_recv()
                agc(j, dx).start()

    def span(p):
        return pl.ds(order[p] * group * R * cap, group * R * cap)

    def gate_up(p):
        for j in members[p]:
            for dx in range(nx):
                agc(j, dx).wait_recv()
        wide = 256 if ff % 256 == 0 else 128

        def piece(i, carry):
            cols = pl.ds(pl.multiple_of(i * wide, wide), wide)
            x = arr[span(p), :]
            g = jnp.dot(x, wg[:, cols], preferred_element_type=f32)
            u = jnp.dot(x, wu[:, cols], preferred_element_type=f32)
            hid[:, cols] = (jax.nn.silu(g) * u).astype(jnp.bfloat16)
            return carry

        lax.fori_loop(0, ff // wide, piece, 0)

    def down(p):
        for j in members[p]:
            for dx in range(nx):
                if dx:
                    agx(j, dx).wait_send()
                agc(j, dx).wait_send()
        wide = 256 if width % 256 == 0 else 128

        def piece(i, carry):
            cols = pl.ds(pl.multiple_of(i * wide, wide), wide)
            arr[span(p), cols] = jnp.dot(
                hid[...], wd[:, cols], preferred_element_type=f32
            ).astype(jnp.bfloat16)
            return carry

        lax.fori_loop(0, width // wide, piece, 0)
        for j in members[p]:
            rsc(j).start()

    def chip_sum(p):
        for j in members[p]:
            rsc(j).wait_recv()
            for dx in range(1, nx):
                both = (
                    arr[rows(j, 0, dx), :].astype(f32)
                    + ra[pl.ds((j * nx + dx) * cap, cap), :].astype(f32)
                )
                sx[pl.ds((j * (nx - 1) + dx - 1) * cap, cap), :] = both.astype(jnp.bfloat16)
                rsx(j, dx).start()

    def finish(p):
        for j in members[p]:
            total = (
                arr[rows(j, 0, 0), :].astype(f32)
                + ra[pl.ds(j * nx * cap, cap), :].astype(f32)
            )
            for dx in range(1, nx):
                rsx(j, dx).wait_recv()
                total = total + rx[pl.ds((j * (nx - 1) + dx - 1) * cap, cap), :].astype(f32)
            if j:
                fin[pl.ds(j * cap, cap), :] = total.astype(jnp.bfloat16)
                back(j).start()
            else:
                ret_ref[pl.ds(0, cap), :] = total.astype(jnp.bfloat16)

    arrive(0)
    loads[0].wait()
    loads[1].wait()
    for p in range(steps):
        relay(p)
        gate_up(p)
        if p + 1 < steps:
            arrive(p + 1)
        if p == 0:
            loads[2].wait()
        if p > 1:
            finish(p - 2)
        if p:
            chip_sum(p - 1)
        down(p)
    if steps > 1:
        finish(steps - 2)
    chip_sum(steps - 1)
    finish(steps - 1)

    for j in range(S):
        rsc(j).wait_send()
        for dx in range(1, nx):
            rsx(j, dx).wait_send()
        if j:
            disp(j).wait_send()
            back(j).wait_send()
            back(j).wait_recv()


def run_experts(outgoing, gate_w, up_w, down_w, S, R, cap):
    width, ff = gate_w.shape
    nx = R // 2
    group = 2
    bf = jnp.bfloat16
    dma = pltpu.SemaphoreType.DMA
    total = S * R * cap
    return pl.pallas_call(
        functools.partial(expert_kernel, S, R, cap, group),
        out_shape=jax.ShapeDtypeStruct((S * cap, width), bf),
        in_specs=[pl.BlockSpec(memory_space=pltpu.VMEM)]
        + [pl.BlockSpec(memory_space=pl.ANY)] * 3,
        out_specs=pl.BlockSpec(memory_space=pltpu.VMEM),
        scratch_shapes=[
            pltpu.VMEM((total, width), bf),
            pltpu.VMEM((group * R * cap, ff), bf),
            pltpu.VMEM((S * nx * cap, width), bf),
            pltpu.VMEM((S * (nx - 1) * cap, width), bf),
            pltpu.VMEM((S * (nx - 1) * cap, width), bf),
            pltpu.VMEM((S * cap, width), bf),
            pltpu.VMEM((width, ff), bf),
            pltpu.VMEM((width, ff), bf),
            pltpu.VMEM((ff, width), bf),
            dma((3,)), dma(()),
            dma((S,)), dma((S,)),
            dma((S, R)), dma((S, R)),
            dma((S,)), dma((S,)),
            dma((S, nx)), dma((S, nx)),
            dma((S,)), dma((S,)),
        ],
        compiler_params=pltpu.CompilerParams(
            collective_id=0, has_side_effects=True, vmem_limit_bytes=58 * 1024 * 1024
        ),
        cost_estimate=pl.CostEstimate(
            flops=6 * total * width * ff, bytes_accessed=6 * width * ff, transcendentals=total * ff
        ),
    )(outgoing, gate_w, up_w, down_w)


def per_device(
    skip_connection_stream,
    emitted_valve_unscaled,
    channel_source_mapped,
    hidden_source_mapped,
    probe_mapped_values,
    increment_premapped,
    extra_log_fading,
    channel_fading_speed,
    channel_source_kernel,
    hidden_source_kernel,
    probe_kernel_coefficients,
    cluster_scaling_factor,
    emitted_mapping_matrix,
    standardize_scaling,
    standardize_offset,
    chosen_specialist_ids,
    specialist_mixing_shares,
    specialist_gating_matrices,
    raising_matrices,
    lowering_matrices,
):
    sp_size = lax.axis_size("sp")
    sp_index = lax.axis_index("sp")
    tok_rows = skip_connection_stream.shape[1]
    model_width = skip_connection_stream.shape[2]
    inner_width = HEADS * HEAD_DIM
    per_group = HEADS // GROUPS
    head_count = HEADS // sp_size
    first_head = sp_index * head_count
    span = max(1, head_count // per_group)
    copies = max(1, per_group // head_count)
    x_part = channel_source_mapped[0].reshape(tok_rows, sp_size, head_count * HEAD_DIM)
    b_part = hidden_source_mapped[0].reshape(tok_rows, GROUPS // span, span * STATE)
    c_part = probe_mapped_values[0].reshape(tok_rows, GROUPS // span, span * STATE)
    payload = jnp.concatenate(
        [x_part, jnp.repeat(b_part, copies, axis=1), jnp.repeat(c_part, copies, axis=1)], axis=2
    )
    sent_width = payload.shape[2]
    arrived = lax.all_to_all(
        payload.reshape(tok_rows, sp_size * sent_width), "sp", split_axis=1, concat_axis=0, tiled=True
    )
    x_width, s_width = head_count * HEAD_DIM, span * STATE
    state_at = (sp_index // copies) * s_width
    taps = jnp.concatenate(
        [
            lax.dynamic_slice_in_dim(channel_source_kernel, sp_index * x_width, x_width, 1),
            lax.dynamic_slice_in_dim(hidden_source_kernel, state_at, s_width, 1),
            lax.dynamic_slice_in_dim(probe_kernel_coefficients, state_at, s_width, 1),
        ],
        axis=1,
    )
    rim_rows = jnp.zeros((KERNEL - 1, sent_width), jnp.bfloat16)
    flat_conv = causal_conv(arrived, taps, rim_rows)
    seq_rows = flat_conv.shape[0]
    x_conv = flat_conv[:, :x_width].reshape(seq_rows, head_count, HEAD_DIM)
    shared = head_count // span
    b_conv = jnp.repeat(
        flat_conv[:, x_width : x_width + s_width].reshape(seq_rows, span, STATE), shared, axis=1
    )
    c_conv = jnp.repeat(
        flat_conv[:, x_width + s_width :].reshape(seq_rows, span, STATE), shared, axis=1
    )
    increment_delta = jax.nn.softplus(increment_premapped[0])
    speeds_per_channel = lax.dynamic_slice_in_dim(channel_fading_speed, first_head, head_count, 0)
    fading_exponent = extra_log_fading[0] - speeds_per_channel[None, :] * increment_delta
    init_state = jnp.zeros((head_count, HEAD_DIM, STATE), jnp.float32)
    outcome, final_state, total_decay = ssd_blocks(
        x_conv,
        b_conv,
        c_conv,
        increment_delta,
        fading_exponent,
        init_state,
        BLK,
    )
    returned_rows = lax.all_to_all(
        outcome.astype(jnp.bfloat16), "sp", split_axis=0, concat_axis=1, tiled=True
    )
    blending_outcome = returned_rows.reshape(tok_rows, inner_width)
    gated = blending_outcome.astype(jnp.float32) * jax.nn.silu(
        emitted_valve_unscaled[0].astype(jnp.float32)
    )
    grouped = gated.reshape(tok_rows, GROUPS, inner_width // GROUPS)
    grouped = grouped * lax.rsqrt(jnp.mean(grouped * grouped, axis=-1, keepdims=True) + rms_eps)
    group_normed = (
        grouped.reshape(tok_rows, inner_width) * cluster_scaling_factor[None, :]
    ).astype(jnp.bfloat16)
    pre_norm = skip_connection_stream[0].astype(jnp.float32) + jnp.dot(
        group_normed, emitted_mapping_matrix, preferred_element_type=jnp.float32
    )
    centre = jnp.mean(pre_norm, axis=-1, keepdims=True)
    variance = jnp.mean(jnp.square(pre_norm - centre), axis=-1, keepdims=True)
    normed = (
        (pre_norm - centre) * lax.rsqrt(variance + norm_eps) * standardize_scaling[None, :]
        + standardize_offset[None, :]
    ).astype(jnp.bfloat16)
    slot_cap = -(-(3 * tok_rows // sp_size) // 16) * 16
    dp_size = lax.axis_size("dp")
    slots = sp_size * slot_cap
    flat_ids = chosen_specialist_ids[0].reshape(-1)
    matched = (flat_ids[:, None] == jnp.arange(sp_size, dtype=jnp.int32)[None, :]).astype(jnp.int32)
    ranked = jnp.cumsum(matched, axis=0) - 1
    relative = jnp.bitwise_xor(flat_ids, sp_index)
    target = (relative * slot_cap + jnp.sum(matched * ranked, axis=1)).reshape(tok_rows, 2)
    placing = jnp.arange(slots, dtype=jnp.int32)[:, None]
    placing = ((placing == target[None, :, 0]) | (placing == target[None, :, 1])).astype(jnp.bfloat16)
    outgoing = jnp.dot(placing, normed, preferred_element_type=jnp.float32).astype(jnp.bfloat16)
    answered = run_experts(
        outgoing,
        specialist_gating_matrices[0],
        raising_matrices[0],
        lowering_matrices[0],
        sp_size,
        dp_size,
        slot_cap,
    )
    slot_index = jnp.arange(slots, dtype=jnp.int32)[None, :]
    routed_sum = jnp.zeros((tok_rows, model_width), jnp.float32)
    for choice in range(2):
        picking = (slot_index == target[:, choice : choice + 1]).astype(jnp.bfloat16)
        routed_sum = routed_sum + specialist_mixing_shares[0][:, choice : choice + 1] * jnp.dot(
            picking, answered, preferred_element_type=jnp.float32
        )
    layer_out = (normed.astype(jnp.float32) + routed_sum).astype(jnp.bfloat16)
    return layer_out[None]


def solution(mesh):
    placed = (
        P("dp", "sp", None),
        P("dp", "sp", None),
        P("dp", "sp", None),
        P("dp", "sp", None),
        P("dp", "sp", None),
        P("dp", None, "sp"),
        P("dp", None, "sp"),
        P(),
        P(),
        P(),
        P(),
        P(),
        P(),
        P(),
        P(),
        P("dp", "sp", None),
        P("dp", "sp", None),
        P("sp", None, "dp"),
        P("sp", None, "dp"),
        P("sp", "dp", None),
    )
    return jax.shard_map(
        per_device, mesh=mesh, in_specs=placed, out_specs=P("dp", "sp", None), check_vma=False
    )
```

```python
import functools

import jax
import jax.numpy as jnp
from jax import lax
from jax.experimental import pallas as pl
from jax.experimental.pallas import tpu as pltpu
from jax.sharding import PartitionSpec as P

HEADS = 16
HEAD_DIM = 64
GROUPS = 4
STATE = 64
KERNEL = 4
BLK = 128


rms_eps = 1e-06
norm_eps = 1e-05


def causal_conv(series, tap_weights, rim_rows):
    padded = jnp.concatenate([rim_rows, series], axis=0).astype(jnp.float32)
    length = series.shape[0]
    running = jnp.zeros(series.shape, jnp.float32)
    for tap_index in range(tap_weights.shape[0]):
        running = running + tap_weights[tap_index] * lax.slice_in_dim(
            padded, tap_index, tap_index + length, axis=0
        )
    return jax.nn.silu(running).astype(jnp.bfloat16)


def ssd_blocks(x_conv, b_conv, c_conv, increment_delta, fading_exponent, init_state, block_len):
    length, head_count, head_width = x_conv.shape
    state_width = b_conv.shape[2]
    block_count = length // block_len
    x_block = x_conv.reshape(block_count, block_len, head_count, head_width)
    b_block = b_conv.reshape(block_count, block_len, head_count, state_width)
    c_block = c_conv.reshape(block_count, block_len, head_count, state_width)
    cumulative = jnp.cumsum(
        jnp.transpose(fading_exponent.reshape(block_count, block_len, head_count), (0, 2, 1)),
        axis=2,
    )
    step_heads = jnp.transpose(
        increment_delta.reshape(block_count, block_len, head_count), (0, 2, 1)
    )
    causal = jnp.arange(block_len)[:, None] >= jnp.arange(block_len)[None, :]
    within = jnp.exp(
        jnp.where(causal, cumulative[:, :, :, None] - cumulative[:, :, None, :], -jnp.inf)
    )
    scores = jnp.einsum("cthn,cshn->chts", c_block, b_block, preferred_element_type=jnp.float32)
    mixing = (scores * within * step_heads[:, :, None, :]).astype(jnp.bfloat16)
    diag_out = jnp.einsum("chts,cshp->cthp", mixing, x_block, preferred_element_type=jnp.float32)
    tail_decay = jnp.exp(cumulative[:, :, -1:] - cumulative) * step_heads
    scaled = (
        x_block.astype(jnp.float32) * jnp.transpose(tail_decay, (0, 2, 1))[:, :, :, None]
    ).astype(jnp.bfloat16)
    block_state = jnp.einsum("cshp,cshn->chpn", scaled, b_block, preferred_element_type=jnp.float32)
    totals = cumulative[:, :, -1]
    through = jnp.cumsum(totals, axis=0)
    before = through - totals
    earlier = jnp.arange(block_count)[:, None] > jnp.arange(block_count)[None, :]
    carry_weight = jnp.exp(
        jnp.where(earlier[:, :, None], before[:, None, :] - through[None, :, :], -jnp.inf)
    )
    entering = (
        jnp.einsum("cjh,jhpn->chpn", carry_weight, block_state, precision=lax.Precision.HIGHEST)
        + jnp.exp(before)[:, :, None, None] * init_state[None]
    )
    reach_decay = jnp.transpose(jnp.exp(cumulative), (0, 2, 1))
    carried_out = (
        jnp.einsum(
            "cthn,chpn->cthp",
            c_block.astype(jnp.float32),
            entering,
            precision=lax.Precision.HIGHEST,
        )
        * reach_decay[:, :, :, None]
    )
    outcome = (diag_out + carried_out).reshape(length, head_count, head_width)
    final_state = (
        jnp.einsum(
            "jh,jhpn->hpn",
            jnp.exp(through[-1][None, :] - through),
            block_state,
            precision=lax.Precision.HIGHEST,
        )
        + jnp.exp(through[-1])[:, None, None] * init_state
    )
    return (outcome, final_state, through[-1])

MESH = pl.DeviceIdType.MESH


def flip(value, mask):
    result, bit = value, 1
    while bit <= mask:
        if mask & bit:
            result = result + bit * (1 - 2 * ((value // bit) % 2))
        bit *= 2
    return result


def expert_kernel(
    S, R, cap, group, out_ref, wg_hbm, wu_hbm, wd_hbm, ret_ref,
    arr, hid, ra, rx, sx, fin, wg, wu, wd,
    wsem, own_sem, d_s, d_r, g_s, g_r, a_s, a_r, x_s, x_r, b_s, b_r,
):
    s = lax.axis_index("sp")
    d = lax.axis_index("dp")
    nx = R // 2
    steps = S // group
    ahead = 2 // group
    order = list(range(ahead)) + list(range(ahead, steps))
    members = [[p * group + i for i in range(group)] for p in order]
    width = wd.shape[1]
    ff = wg.shape[1]
    f32 = jnp.float32

    def rows(j, dc, dx, count=1):
        return pl.ds((j * R + dc * nx + dx) * cap, count * cap)

    def remote(src, dst, send, recv, where):
        return pltpu.make_async_remote_copy(
            src_ref=src, dst_ref=dst, send_sem=send, recv_sem=recv,
            device_id=where, device_id_type=MESH,
        )

    def disp(j):
        return remote(out_ref.at[pl.ds(j * cap, cap)], arr.at[rows(j, 0, 0)],
                      d_s.at[j], d_r.at[j], {"sp": flip(s, j)})

    def agx(j, dx):
        return remote(arr.at[rows(j, 0, 0)], arr.at[rows(j, 0, dx)],
                      g_s.at[j, dx], g_r.at[j, dx], {"dp": flip(d, 2 * dx)})

    def agc(j, dx):
        return remote(arr.at[rows(j, 0, dx)], arr.at[rows(j, 1, dx)],
                      g_s.at[j, nx + dx], g_r.at[j, nx + dx], {"dp": flip(d, 1)})

    def rsc(j):
        return remote(arr.at[rows(j, 1, 0, nx)], ra.at[pl.ds(j * nx * cap, nx * cap)],
                      a_s.at[j], a_r.at[j], {"dp": flip(d, 1)})

    def rsx(j, dx):
        at = pl.ds((j * (nx - 1) + dx - 1) * cap, cap)
        return remote(sx.at[at], rx.at[at], x_s.at[j, dx], x_r.at[j, dx], {"dp": flip(d, 2 * dx)})

    def back(j):
        return remote(fin.at[pl.ds(j * cap, cap)], ret_ref.at[pl.ds(j * cap, cap)],
                      b_s.at[j], b_r.at[j], {"sp": flip(s, j)})

    own = pltpu.make_async_copy(out_ref.at[pl.ds(0, cap)], arr.at[rows(0, 0, 0)], own_sem)
    loads = [
        pltpu.make_async_copy(src, dst, wsem.at[i])
        for i, (src, dst) in enumerate(((wg_hbm, wg), (wu_hbm, wu), (wd_hbm, wd)))
    ]
    own.start()
    for load in loads:
        load.start()

    barrier = pltpu.get_barrier_semaphore()
    peers = [{"sp": flip(s, j)} for j in range(1, S)]
    peers += [{"dp": flip(d, 1)}] + [{"dp": flip(d, 2 * dx)} for dx in range(1, nx)]
    for peer in peers:
        pl.semaphore_signal(barrier, inc=1, device_id=peer, device_id_type=MESH)
    pl.semaphore_wait(barrier, len(peers))

    for js in members:
        for j in js:
            if j:
                disp(j).start()

    def arrive(p):
        for j in members[p]:
            if j:
                disp(j).wait_recv()
            else:
                own.wait()
            for dx in range(1, nx):
                agx(j, dx).start()
            agc(j, 0).start()

    def relay(p):
        for j in members[p]:
            for dx in range(1, nx):
                agx(j, dx).wait_recv()
                agc(j, dx).start()

    def span(p):
        return pl.ds(order[p] * group * R * cap, group * R * cap)

    def gate_up(p):
        for j in members[p]:
            for dx in range(nx):
                agc(j, dx).wait_recv()
        wide = 256 if ff % 256 == 0 else 128

        def piece(i, carry):
            cols = pl.ds(pl.multiple_of(i * wide, wide), wide)
            x = arr[span(p), :]
            g = jnp.dot(x, wg[:, cols], preferred_element_type=f32)
            u = jnp.dot(x, wu[:, cols], preferred_element_type=f32)
            hid[:, cols] = (jax.nn.silu(g) * u).astype(jnp.bfloat16)
            return carry

        lax.fori_loop(0, ff // wide, piece, 0)

    def down(p):
        for j in members[p]:
            for dx in range(nx):
                if dx:
                    agx(j, dx).wait_send()
                agc(j, dx).wait_send()
        wide = 256 if width % 256 == 0 else 128

        def piece(i, carry):
            cols = pl.ds(pl.multiple_of(i * wide, wide), wide)
            arr[span(p), cols] = jnp.dot(
                hid[...], wd[:, cols], preferred_element_type=f32
            ).astype(jnp.bfloat16)
            return carry

        lax.fori_loop(0, width // wide, piece, 0)
        for j in members[p]:
            rsc(j).start()

    def chip_sum(p):
        for j in members[p]:
            rsc(j).wait_recv()
            for dx in range(1, nx):
                both = (
                    arr[rows(j, 0, dx), :].astype(f32)
                    + ra[pl.ds((j * nx + dx) * cap, cap), :].astype(f32)
                )
                sx[pl.ds((j * (nx - 1) + dx - 1) * cap, cap), :] = both.astype(jnp.bfloat16)
                rsx(j, dx).start()

    def finish(p):
        for j in members[p]:
            total = (
                arr[rows(j, 0, 0), :].astype(f32)
                + ra[pl.ds(j * nx * cap, cap), :].astype(f32)
            )
            for dx in range(1, nx):
                rsx(j, dx).wait_recv()
                total = total + rx[pl.ds((j * (nx - 1) + dx - 1) * cap, cap), :].astype(f32)
            if j:
                fin[pl.ds(j * cap, cap), :] = total.astype(jnp.bfloat16)
                back(j).start()
            else:
                ret_ref[pl.ds(0, cap), :] = total.astype(jnp.bfloat16)

    for p in range(ahead):
        arrive(p)
    loads[0].wait()
    loads[1].wait()
    for p in range(steps):
        relay(p)
        gate_up(p)
        if p + ahead < steps:
            arrive(p + ahead)
        if p == 0:
            loads[2].wait()
        if p > 1:
            finish(p - 2)
        if p:
            chip_sum(p - 1)
        down(p)
    if steps > 1:
        finish(steps - 2)
    chip_sum(steps - 1)
    finish(steps - 1)

    for j in range(S):
        rsc(j).wait_send()
        for dx in range(1, nx):
            rsx(j, dx).wait_send()
        if j:
            disp(j).wait_send()
            back(j).wait_send()
            back(j).wait_recv()


def run_experts(outgoing, gate_w, up_w, down_w, S, R, cap):
    width, ff = gate_w.shape
    nx = R // 2
    group = 1
    bf = jnp.bfloat16
    dma = pltpu.SemaphoreType.DMA
    total = S * R * cap
    return pl.pallas_call(
        functools.partial(expert_kernel, S, R, cap, group),
        out_shape=jax.ShapeDtypeStruct((S * cap, width), bf),
        in_specs=[pl.BlockSpec(memory_space=pltpu.VMEM)]
        + [pl.BlockSpec(memory_space=pl.ANY)] * 3,
        out_specs=pl.BlockSpec(memory_space=pltpu.VMEM),
        scratch_shapes=[
            pltpu.VMEM((total, width), bf),
            pltpu.VMEM((group * R * cap, ff), bf),
            pltpu.VMEM((S * nx * cap, width), bf),
            pltpu.VMEM((S * (nx - 1) * cap, width), bf),
            pltpu.VMEM((S * (nx - 1) * cap, width), bf),
            pltpu.VMEM((S * cap, width), bf),
            pltpu.VMEM((width, ff), bf),
            pltpu.VMEM((width, ff), bf),
            pltpu.VMEM((ff, width), bf),
            dma((3,)), dma(()),
            dma((S,)), dma((S,)),
            dma((S, R)), dma((S, R)),
            dma((S,)), dma((S,)),
            dma((S, nx)), dma((S, nx)),
            dma((S,)), dma((S,)),
        ],
        compiler_params=pltpu.CompilerParams(
            collective_id=0, has_side_effects=True, vmem_limit_bytes=58 * 1024 * 1024
        ),
        cost_estimate=pl.CostEstimate(
            flops=6 * total * width * ff, bytes_accessed=6 * width * ff, transcendentals=total * ff
        ),
    )(outgoing, gate_w, up_w, down_w)


def per_device(
    skip_connection_stream,
    emitted_valve_unscaled,
    channel_source_mapped,
    hidden_source_mapped,
    probe_mapped_values,
    increment_premapped,
    extra_log_fading,
    channel_fading_speed,
    channel_source_kernel,
    hidden_source_kernel,
    probe_kernel_coefficients,
    cluster_scaling_factor,
    emitted_mapping_matrix,
    standardize_scaling,
    standardize_offset,
    chosen_specialist_ids,
    specialist_mixing_shares,
    specialist_gating_matrices,
    raising_matrices,
    lowering_matrices,
):
    sp_size = lax.axis_size("sp")
    sp_index = lax.axis_index("sp")
    tok_rows = skip_connection_stream.shape[1]
    model_width = skip_connection_stream.shape[2]
    inner_width = HEADS * HEAD_DIM
    per_group = HEADS // GROUPS
    head_count = HEADS // sp_size
    first_head = sp_index * head_count
    span = max(1, head_count // per_group)
    copies = max(1, per_group // head_count)
    x_part = channel_source_mapped[0].reshape(tok_rows, sp_size, head_count * HEAD_DIM)
    b_part = hidden_source_mapped[0].reshape(tok_rows, GROUPS // span, span * STATE)
    c_part = probe_mapped_values[0].reshape(tok_rows, GROUPS // span, span * STATE)
    payload = jnp.concatenate(
        [x_part, jnp.repeat(b_part, copies, axis=1), jnp.repeat(c_part, copies, axis=1)], axis=2
    )
    sent_width = payload.shape[2]
    arrived = lax.all_to_all(
        payload.reshape(tok_rows, sp_size * sent_width), "sp", split_axis=1, concat_axis=0, tiled=True
    )
    x_width, s_width = head_count * HEAD_DIM, span * STATE
    state_at = (sp_index // copies) * s_width
    taps = jnp.concatenate(
        [
            lax.dynamic_slice_in_dim(channel_source_kernel, sp_index * x_width, x_width, 1),
            lax.dynamic_slice_in_dim(hidden_source_kernel, state_at, s_width, 1),
            lax.dynamic_slice_in_dim(probe_kernel_coefficients, state_at, s_width, 1),
        ],
        axis=1,
    )
    rim_rows = jnp.zeros((KERNEL - 1, sent_width), jnp.bfloat16)
    flat_conv = causal_conv(arrived, taps, rim_rows)
    seq_rows = flat_conv.shape[0]
    x_conv = flat_conv[:, :x_width].reshape(seq_rows, head_count, HEAD_DIM)
    shared = head_count // span
    b_conv = jnp.repeat(
        flat_conv[:, x_width : x_width + s_width].reshape(seq_rows, span, STATE), shared, axis=1
    )
    c_conv = jnp.repeat(
        flat_conv[:, x_width + s_width :].reshape(seq_rows, span, STATE), shared, axis=1
    )
    increment_delta = jax.nn.softplus(increment_premapped[0])
    speeds_per_channel = lax.dynamic_slice_in_dim(channel_fading_speed, first_head, head_count, 0)
    fading_exponent = extra_log_fading[0] - speeds_per_channel[None, :] * increment_delta
    init_state = jnp.zeros((head_count, HEAD_DIM, STATE), jnp.float32)
    outcome, final_state, total_decay = ssd_blocks(
        x_conv,
        b_conv,
        c_conv,
        increment_delta,
        fading_exponent,
        init_state,
        BLK,
    )
    returned_rows = lax.all_to_all(
        outcome.astype(jnp.bfloat16).reshape(sp_size, tok_rows, x_width),
        "sp",
        split_axis=0,
        concat_axis=0,
        tiled=True,
    )
    blending_outcome = jnp.concatenate([returned_rows[i] for i in range(sp_size)], axis=1)
    gated = blending_outcome.astype(jnp.float32) * jax.nn.silu(
        emitted_valve_unscaled[0].astype(jnp.float32)
    )
    grouped = gated.reshape(tok_rows, GROUPS, inner_width // GROUPS)
    grouped = grouped * lax.rsqrt(jnp.mean(grouped * grouped, axis=-1, keepdims=True) + rms_eps)
    group_normed = (
        grouped.reshape(tok_rows, inner_width) * cluster_scaling_factor[None, :]
    ).astype(jnp.bfloat16)
    pre_norm = skip_connection_stream[0].astype(jnp.float32) + jnp.dot(
        group_normed, emitted_mapping_matrix, preferred_element_type=jnp.float32
    )
    centre = jnp.mean(pre_norm, axis=-1, keepdims=True)
    variance = jnp.mean(jnp.square(pre_norm - centre), axis=-1, keepdims=True)
    normed = (
        (pre_norm - centre) * lax.rsqrt(variance + norm_eps) * standardize_scaling[None, :]
        + standardize_offset[None, :]
    ).astype(jnp.bfloat16)
    slot_cap = -(-(3 * tok_rows // sp_size) // 16) * 16
    dp_size = lax.axis_size("dp")
    slots = sp_size * slot_cap
    flat_ids = chosen_specialist_ids[0].reshape(-1)
    matched = (flat_ids[:, None] == jnp.arange(sp_size, dtype=jnp.int32)[None, :]).astype(jnp.int32)
    ranked = jnp.cumsum(matched, axis=0) - 1
    relative = jnp.bitwise_xor(flat_ids, sp_index)
    target = (relative * slot_cap + jnp.sum(matched * ranked, axis=1)).reshape(tok_rows, 2)
    placing = jnp.arange(slots, dtype=jnp.int32)[:, None]
    placing = ((placing == target[None, :, 0]) | (placing == target[None, :, 1])).astype(jnp.bfloat16)
    outgoing = jnp.dot(placing, normed, preferred_element_type=jnp.float32).astype(jnp.bfloat16)
    answered = run_experts(
        outgoing,
        specialist_gating_matrices[0],
        raising_matrices[0],
        lowering_matrices[0],
        sp_size,
        dp_size,
        slot_cap,
    )
    slot_index = jnp.arange(slots, dtype=jnp.int32)[None, :]
    routed_sum = jnp.zeros((tok_rows, model_width), jnp.float32)
    for choice in range(2):
        picking = (slot_index == target[:, choice : choice + 1]).astype(jnp.bfloat16)
        routed_sum = routed_sum + specialist_mixing_shares[0][:, choice : choice + 1] * jnp.dot(
            picking, answered, preferred_element_type=jnp.float32
        )
    layer_out = (normed.astype(jnp.float32) + routed_sum).astype(jnp.bfloat16)
    return layer_out[None]


def solution(mesh):
    placed = (
        P("dp", "sp", None),
        P("dp", "sp", None),
        P("dp", "sp", None),
        P("dp", "sp", None),
        P("dp", "sp", None),
        P("dp", None, "sp"),
        P("dp", None, "sp"),
        P(),
        P(),
        P(),
        P(),
        P(),
        P(),
        P(),
        P(),
        P("dp", "sp", None),
        P("dp", "sp", None),
        P("sp", None, "dp"),
        P("sp", None, "dp"),
        P("sp", "dp", None),
    )
    return jax.shard_map(
        per_device, mesh=mesh, in_specs=placed, out_specs=P("dp", "sp", None), check_vma=False
    )
```
